32 devices in a mesh: ep: 4 (over y, x), tp: 8 (over z, core).
Axes of the slice: x: 2, y: 2, z: 4, core: 2. Of those that a mesh axis runs over, the one named last changes fastest.
Arguments:
- tokens: bfloat16 [4096, 2048], P('ep', 'tp'), may hold values from -48 to 48
- pre_gain: bfloat16 [2048], P('tp'), may hold values from 0.099609375 to 1.8984375
- route_ids: int32 [4096, 2], P('ep'), may hold values from 0 to 3, all different within a row; in each aligned block of 1024 rows (0 to 1023, 1024 to 2047, ...) at most 576 rows name the same one
- route_weights: float32 [4096, 2], P('ep'), may hold values from 0.1 to 1
- gate_weight: bfloat16 [4, 2048, 7168], P('ep', None, 'tp'), may hold values from -0.125 to 0.125
- up_weight: bfloat16 [4, 2048, 7168], P('ep', None, 'tp'), may hold values from -0.125 to 0.125
- down_weight: bfloat16 [4, 7168, 2048], P('ep', 'tp')
- post_gain: bfloat16 [2048], P('tp'), may hold values from 0.099609375 to 1.8984375
Outputs:
- mixed: bfloat16 [4096, 2048], P('ep', 'tp')
The draws below stay inside these ranges and needn't reach their ends.
Inputs may be any that keep to these rules, and one draw needn't show every extreme that they name: `route_ids`: each row names 2 different experts; among the rows of one index of ep no expert is named more than 576 times, a bound that some block reaches.
All inputs are finite; a program needn't handle non-finite values.
Results may differ from the reference program's by a relative error of at most 0.02.
Values may be sent and summed in bfloat16 or wider, within the bound.
A program may use at most 128 MiB of HBM per device.

```python
import math
import jax
import jax.numpy as jnp
import numpy as np
from jax import lax

D = 2048
FF = 7168
TOP = 2
TOK_DEV = 1024
EXPERTS = 4
TOKENS = 4096
CAP = 576
N_EP = 4
N_TP = 8


def column_profile(key):
    position = jnp.arange(D, dtype=jnp.float32) / D
    return 0.5 * jnp.exp(math.log(4.0) * position) * jax.random.uniform(key, (D,), jnp.float32, 0.6, 1.4)


def draw_tokens(key, part):
    first, second, third = jax.random.split(jax.random.fold_in(key, 11), 3)
    columns = column_profile(second)
    base = jnp.clip(jax.random.normal(first, (TOKENS, D), jnp.float32), -5.0, 5.0)
    row_scale = jnp.exp(jax.random.uniform(third, (TOKENS, 1), jnp.float32, math.log(0.3), math.log(3.0)))
    return (base * row_scale * columns[None, :]).astype(jnp.bfloat16)


def draw_down_weight(key, part):
    first, second = jax.random.split(jax.random.fold_in(key, 23), 2)
    columns = column_profile(second)
    base = jnp.clip(jax.random.normal(first, (EXPERTS, FF, D), jnp.float32), -5.0, 5.0)
    return (base * FF ** (-0.5) * columns[None, None, :]).astype(jnp.bfloat16)


def block_scale(rng, shape, cuts, least, top_value):
    def one(axis_at, parts):
        heights = jax.random.uniform(jax.random.fold_in(jax.random.fold_in(rng, 6), axis_at), (parts,), jnp.float32, least / len(cuts), top_value / len(cuts))
        return jnp.repeat(jnp.exp(heights), shape[axis_at] // parts).reshape((-1,) + (1,) * (len(shape) - axis_at - 1))

    factor_of = one(*cuts[0])
    for cut in cuts[1:]:
        factor_of = factor_of * one(*cut)
    return factor_of


def routed_block(key, own, number, rows, amount, top, most, skew):
    sequence = jax.random.permutation(key, amount)
    crowded, ordinary = portions_of(amount, rows * top, most, skew, True), portions_of(amount, rows * top, most, skew, False)
    places = jnp.arange(amount)

    def named(lengths, rotation):
        used = int((lengths > 0).sum())
        fixed = max(1, used // 4)
        passed = fixed + (places - fixed + rotation * (used - fixed)) % max(1, amount - fixed)
        return jnp.zeros((amount,), jnp.int32).at[sequence[jnp.where(places < fixed, places, passed)]].set(jnp.asarray(lengths, jnp.int32))

    lengths = jnp.where(number % 4 == 0, named(crowded, number // 4), named(ordinary, number - number // 4 - 1))
    mixed = jax.random.permutation(jax.random.fold_in(own, 3), amount)
    donor, receiver = mixed[0:amount // 2 * 2:2], mixed[1:amount // 2 * 2:2]
    room = jnp.minimum(lengths[donor] - 1, most - lengths[receiver]) // 2
    room = jnp.where((donor == sequence[0]) | (receiver == sequence[0]) | (lengths[receiver] == 0), 0, jnp.maximum(room, 0))
    passed = jax.random.randint(jax.random.fold_in(own, 4), (amount // 2,), 0, 1 << 20) % (room + 1)
    lengths = lengths.at[donor].add(-passed).at[receiver].add(passed)
    labels = jnp.searchsorted(jnp.cumsum(lengths), jnp.arange(rows * top), side="right").astype(jnp.int32)
    table = labels.reshape(top, rows).T
    table = table[jax.random.permutation(jax.random.fold_in(own, 1), rows)]
    rotation = jax.random.randint(jax.random.fold_in(own, 2), (rows, 1), 0, top)
    return jnp.take_along_axis(table, (jnp.arange(top)[None, :] + rotation) % top, axis=1)


def portions_of(amount, total, most, skew, full):
    loads = [(1 << 20) // math.isqrt(rank ** skew) + 1 for rank in range(1, amount + 1)]
    largest = most if full else min(most, max(-(-total // amount), total * loads[0] // sum(loads)))
    least = 1 if total - largest >= amount - 1 else 0
    counts, spare = [largest] + [least] * (amount - 1), total - largest - least * (amount - 1)
    while spare > 0:
        free = [i for i in range(1, amount) if counts[i] < largest] or [i for i in range(1, amount) if counts[i] < most]
        pool, budget = sum([loads[i] for i in free]), spare
        for i in free:
            addition = min(most - counts[i], max(1, budget * loads[i] // pool), spare)
            counts[i] = counts[i] + addition
            spare = spare - addition
    return np.array(counts)


def noise(stream_key, shape, deviation, most, pieces=(), kind=jnp.bfloat16):
    array = deviation * jax.random.normal(stream_key, shape, jnp.float32)
    if pieces:
        array = array * block_scale(stream_key, shape, pieces, -0.22, 0.18)
    return jnp.clip(array, -most, most).astype(kind)


def setup_inputs(seed: int = 0) -> dict:
    keys = jax.random.split(jax.random.key(seed), 9)
    tokens = draw_tokens(jax.random.fold_in(keys[8], 71), 0)
    pre_gain = jnp.clip(1.0 + 0.18 * jax.random.normal(keys[1], (D,), jnp.float32), 0.099609375, 1.8984375).astype(jnp.bfloat16)
    route_ids_keys = jax.random.split(jax.random.fold_in(keys[2], 1), TOKENS // TOK_DEV)
    route_ids_turns = jax.random.permutation(jax.random.fold_in(keys[2], 3), TOKENS // TOK_DEV)
    route_ids = jax.vmap(lambda own, number: routed_block(jax.random.fold_in(keys[2], 2), own, number, TOK_DEV, EXPERTS, TOP, CAP, 2))(route_ids_keys, route_ids_turns).reshape((TOKENS, TOP))
    route_weights = jnp.clip(jnp.exp(math.log(1.0) - 2.3025851 * jax.random.uniform(keys[3], (TOKENS, TOP), jnp.float32) ** block_scale(keys[3], (TOKENS, TOP), ((0, 4),), -0.2, 0.2)), 0.1, 1.0)
    gate_weight = noise(keys[4], (EXPERTS, D, FF), D ** -0.5, 0.125, ((0, 4), (2, 8)))
    up_weight = noise(keys[5], (EXPERTS, D, FF), D ** -0.5, 0.125, ((0, 4), (2, 8)))
    down_weight = draw_down_weight(jax.random.fold_in(keys[8], 71), 0)
    post_gain = jnp.clip(1.0 + 0.18 * jax.random.normal(keys[7], (D,), jnp.float32), 0.099609375, 1.8984375).astype(jnp.bfloat16)
    return dict(tokens=tokens, pre_gain=pre_gain, route_ids=route_ids, route_weights=route_weights, gate_weight=gate_weight, up_weight=up_weight, down_weight=down_weight, post_gain=post_gain)


epsilon = 1e-06

def reference(tokens, pre_gain, route_ids, route_weights, gate_weight, up_weight, down_weight, post_gain):
    values = tokens.astype(jnp.float32)
    normed = (values * lax.rsqrt(lax.optimization_barrier(jnp.mean(values * values, axis=1, keepdims=True)) + epsilon) * pre_gain.astype(jnp.float32)).astype(jnp.bfloat16)
    tok_total = tokens.shape[0]
    rows_total = N_EP * CAP
    hidden_units = FF // N_TP
    flat_ids = route_ids.reshape(-1).astype(jnp.int32)
    onehot = (flat_ids[:, None] == jnp.arange(EXPERTS, dtype=jnp.int32)[None, :]).astype(jnp.int32)
    slot_rank = lax.optimization_barrier(jnp.sum((jnp.cumsum(onehot, axis=0) - 1) * onehot, axis=1)).astype(jnp.int32)
    padded = jnp.concatenate([normed, jnp.zeros((1, D), jnp.bfloat16)], axis=0)
    positions = jnp.arange(tok_total * TOP, dtype=jnp.int32)

    def one_expert(expert):
        target = jnp.where(flat_ids == expert, slot_rank, rows_total).astype(jnp.int32)
        slot_table = jnp.full((rows_total,), tok_total * TOP, jnp.int32).at[target].set(positions, mode='drop')
        routed = padded[slot_table // TOP]
        gate_act = jnp.dot(routed, gate_weight[expert], preferred_element_type=jnp.float32)
        up_act = jnp.dot(routed, up_weight[expert], preferred_element_type=jnp.float32)
        hidden = (jax.nn.silu(gate_act) * up_act).astype(jnp.bfloat16)
        partials = jnp.einsum('rjf,jfd->jrd', hidden.reshape(rows_total, N_TP, hidden_units).astype(jnp.float32), down_weight[expert].reshape(N_TP, hidden_units, D).astype(jnp.float32))
        partials = lax.optimization_barrier(partials.astype(jnp.bfloat16)).astype(jnp.float32)
        return lax.optimization_barrier(jnp.sum(partials, axis=0)).astype(jnp.bfloat16)
    results = lax.map(one_expert, jnp.arange(EXPERTS, dtype=jnp.int32))
    copies = results.reshape(EXPERTS * rows_total, D)[flat_ids * rows_total + slot_rank]
    copies = copies.astype(jnp.float32).reshape(tok_total, TOP, D)
    combined = lax.optimization_barrier(jnp.sum(copies * route_weights[:, :, None], axis=1))
    scaled = combined * lax.rsqrt(lax.optimization_barrier(jnp.mean(combined * combined, axis=1, keepdims=True)) + epsilon)
    return (scaled * post_gain.astype(jnp.float32)).astype(jnp.bfloat16)
```

```python
import functools

import jax
import jax.numpy as jnp
from jax import lax
from jax.experimental import pallas as pl
from jax.experimental.pallas import tpu as pltpu
from jax.sharding import PartitionSpec as P

epsilon = 1e-06
MESH = pl.DeviceIdType.MESH
DMA = pltpu.SemaphoreType.DMA
BF16 = jnp.bfloat16


def greet(targets):
    barrier = pltpu.get_barrier_semaphore()
    for target in targets:
        pl.semaphore_signal(barrier, inc=1, device_id=target, device_id_type=MESH)
    pl.semaphore_wait(barrier, len(targets))


def exchange_kernel(n, x_ref, out_ref, buf, send, recv):
    me = lax.axis_index("tp")
    peers = [{"tp": lax.rem(me + k, n)} for k in range(1, n)]
    greet(peers)
    copies = []
    for k in range(1, n):
        copy = pltpu.make_async_remote_copy(
            src_ref=x_ref, dst_ref=buf.at[k - 1], send_sem=send.at[k - 1],
            recv_sem=recv.at[k - 1], device_id=peers[k - 1], device_id_type=MESH,
        )
        copy.start()
        copies.append(copy)
    total = x_ref[...]
    for k in range(1, n):
        copies[k - 1].wait_recv()
        total = total + buf[k - 1]
    out_ref[...] = total
    for copy in copies:
        copy.wait_send()


def sum_over_tp(rows, number):
    n = lax.axis_size("tp")
    x = rows.reshape(-1, 128)
    total = pl.pallas_call(
        functools.partial(exchange_kernel, n),
        out_shape=jax.ShapeDtypeStruct(x.shape, jnp.float32),
        in_specs=[pl.BlockSpec(memory_space=pltpu.VMEM)],
        out_specs=pl.BlockSpec(memory_space=pltpu.VMEM),
        scratch_shapes=[pltpu.VMEM((n - 1,) + x.shape, jnp.float32), DMA((n - 1,)), DMA((n - 1,))],
        compiler_params=pltpu.CompilerParams(collective_id=number, has_side_effects=True),
        name="exchange%d" % number,
    )(x)
    return total.reshape(-1)


def places(groups, layers):
    me, g = lax.axis_index("tp"), lax.axis_index("ep")
    core, z = lax.rem(me, 2), me // 2
    return core, z, g, {"tp": me + 1 - 2 * core}


def greet_all(groups, layers, core, z, g, partner):
    targets = [partner]
    targets += [{"tp": lax.rem(z + k, layers) * 2 + core} for k in range(1, layers)]
    targets += [{"ep": lax.rem(g + m, groups)} for m in range(1, groups)]
    greet(targets)


def dispatch_kernel(
    groups, layers, cap, cols, x_ref, s_ref, out_ref, zbuf, obuf, zs, zr, es, er, ds, dr, ls
):
    core, z, g, partner = places(groups, layers)
    greet_all(groups, layers, core, z, g, partner)

    def z_copy(k):
        return pltpu.make_async_remote_copy(
            src_ref=x_ref, dst_ref=zbuf.at[k], send_sem=zs.at[k], recv_sem=zr.at[k],
            device_id={"tp": lax.rem(z + k, layers) * 2 + core}, device_id_type=MESH,
        )

    def area(k, m, of):
        source = lax.rem(g + groups - m, groups)
        column = (lax.rem(z + layers - k, layers) * 2 + of) * cols
        return out_ref.at[
            pl.ds(pl.multiple_of(source * cap, 16), cap), pl.ds(pl.multiple_of(column, 128), cols)
        ]

    def e_copy(k, m):
        return pltpu.make_async_remote_copy(
            src_ref=obuf.at[k, m], dst_ref=area(k, 0, core), send_sem=es.at[k, m],
            recv_sem=er.at[k, m], device_id={"ep": lax.rem(g + m, groups)}, device_id_type=MESH,
        )

    def d_copy(k, m, source):
        return pltpu.make_async_remote_copy(
            src_ref=source, dst_ref=area(k, m, core), send_sem=ds.at[k, m],
            recv_sem=dr.at[k, m], device_id=partner, device_id_type=MESH,
        )

    def l_copy(k):
        return pltpu.make_async_copy(obuf.at[k, 0], area(k, 0, core), ls.at[k])

    for k in range(1, layers):
        z_copy(k).start()
    zbuf[0] = x_ref[...]

    def forward(k):
        @pl.loop(1, groups)
        def _(m):
            e_copy(k, m).wait_recv()
            d_copy(k, m, area(k, m, core)).start()

    @pl.loop(0, layers)
    def _(k):
        @pl.when(k > 0)
        def _():
            z_copy(k).wait_recv()

        @pl.loop(0, groups)
        def _(i):
            m = lax.rem(i + 1, groups)
            obuf[k, m] = jnp.dot(
                s_ref[lax.rem(g + m, groups)], zbuf[k], preferred_element_type=jnp.float32
            ).astype(BF16)

            @pl.when(m > 0)
            def _():
                e_copy(k, m).start()

        l_copy(k).start()
        d_copy(k, 0, obuf.at[k, 0]).start()

        @pl.when(k > 0)
        def _():
            forward(k - 1)

    forward(layers - 1)

    @pl.loop(0, layers)
    def _(k):
        @pl.when(k > 0)
        def _():
            z_copy(k).wait_send()

        l_copy(k).wait()

        @pl.loop(0, groups)
        def _(m):
            @pl.when(m > 0)
            def _():
                e_copy(k, m).wait_send()

            copy = d_copy(k, m, obuf.at[k, 0])
            copy.wait_send()
            copy.wait_recv()


def dispatch(normed, table):
    groups, cap, tok_rows = table.shape
    layers = lax.axis_size("tp") // 2
    cols = normed.shape[1]
    vmem = pl.BlockSpec(memory_space=pltpu.VMEM)
    return pl.pallas_call(
        functools.partial(dispatch_kernel, groups, layers, cap, cols),
        out_shape=jax.ShapeDtypeStruct((groups * cap, 2 * layers * cols), BF16),
        in_specs=[vmem, vmem],
        out_specs=pl.BlockSpec(memory_space=pl.ANY),
        scratch_shapes=[
            pltpu.VMEM((layers, tok_rows, cols), BF16),
            pltpu.VMEM((layers, groups, cap, cols), BF16),
            DMA((layers,)), DMA((layers,)),
            DMA((layers, groups)), DMA((layers, groups)),
            DMA((layers, groups)), DMA((layers, groups)),
            DMA((layers,)),
        ],
        compiler_params=pltpu.CompilerParams(
            collective_id=1, has_side_effects=True, vmem_limit_bytes=56 * 2**20
        ),
        name="dispatch",
    )(normed, table)


def return_kernel(
    groups, layers, cap, cols, p_ref, w_ref, out_ref, lbuf, pbuf, qbuf, rbuf, obuf, fbuf,
    ls, ds, dr, es, er, zs, zr,
):
    core, z, g, partner = places(groups, layers)
    greet_all(groups, layers, core, z, g, partner)
    rows = groups * cap

    def columns(k, of):
        column = (lax.rem(z + k, layers) * 2 + of) * cols
        return p_ref.at[:, pl.ds(pl.multiple_of(column, 128), cols)]

    def l_copy(k):
        return pltpu.make_async_copy(columns(k, core), lbuf.at[k], ls.at[k])

    def d_copy(k):
        return pltpu.make_async_remote_copy(
            src_ref=columns(k, 1 - core), dst_ref=pbuf.at[k], send_sem=ds.at[k],
            recv_sem=dr.at[k], device_id=partner, device_id_type=MESH,
        )

    def e_copy(k, m):
        return pltpu.make_async_remote_copy(
            src_ref=qbuf.at[k, m], dst_ref=rbuf.at[k, pl.ds(pl.multiple_of(g * cap, 16), cap)],
            send_sem=es.at[k, m], recv_sem=er.at[k, m],
            device_id={"ep": lax.rem(g + m, groups)}, device_id_type=MESH,
        )

    def z_copy(k):
        return pltpu.make_async_remote_copy(
            src_ref=obuf.at[k], dst_ref=fbuf.at[k], send_sem=zs.at[k], recv_sem=zr.at[k],
            device_id={"tp": lax.rem(z + k, layers) * 2 + core}, device_id_type=MESH,
        )

    @pl.loop(0, layers)
    def _(i):
        k = lax.rem(i + 1, layers)
        d_copy(k).start()
        l_copy(k).start()

    @pl.loop(0, layers)
    def _(i):
        k = lax.rem(i + 1, layers)
        l_copy(k).wait()
        d_copy(k).wait_recv()

        @pl.loop(0, groups)
        def _(j):
            m = lax.rem(j + 1, groups)
            at = pl.ds(pl.multiple_of(lax.rem(g + m, groups) * cap, 16), cap)
            both = lbuf[k, at].astype(jnp.float32) + pbuf[k, at].astype(jnp.float32)

            @pl.when(m > 0)
            def _():
                qbuf[k, m] = both.astype(BF16)
                e_copy(k, m).start()

            @pl.when(m == 0)
            def _():
                rbuf[k, pl.ds(pl.multiple_of(g * cap, 16), cap)] = both.astype(BF16)

    tok_rows = w_ref.shape[0]
    tile = min(256, tok_rows)

    @pl.loop(0, layers)
    def _(i):
        k = lax.rem(i + 1, layers)

        @pl.loop(1, groups)
        def _(m):
            e_copy(k, m).wait_recv()

        @pl.loop(0, tok_rows // tile)
        def _(t):
            at = pl.ds(pl.multiple_of(t * tile, tile), tile)
            value = jnp.dot(w_ref[at], rbuf[k], preferred_element_type=jnp.float32)

            @pl.when(k > 0)
            def _():
                obuf[k, at] = value.astype(BF16)

            @pl.when(k == 0)
            def _():
                out_ref[at] = value

        @pl.when(k > 0)
        def _():
            z_copy(k).start()

    @pl.loop(1, layers)
    def _(k):
        z_copy(k).wait_recv()
        out_ref[...] += fbuf[k].astype(jnp.float32)

    @pl.loop(0, layers)
    def _(k):
        d_copy(k).wait_send()

        @pl.loop(1, groups)
        def _(m):
            e_copy(k, m).wait_send()

        @pl.when(k > 0)
        def _():
            z_copy(k).wait_send()


def give_back(partials, mixing, groups):
    rows, width = partials.shape
    tok_rows = mixing.shape[0]
    layers = lax.axis_size("tp") // 2
    cols = width // (2 * layers)
    cap = rows // groups
    vmem = pl.BlockSpec(memory_space=pltpu.VMEM)
    return pl.pallas_call(
        functools.partial(return_kernel, groups, layers, cap, cols),
        out_shape=jax.ShapeDtypeStruct((tok_rows, cols), jnp.float32),
        in_specs=[pl.BlockSpec(memory_space=pl.ANY), vmem],
        out_specs=vmem,
        scratch_shapes=[
            pltpu.VMEM((layers, rows, cols), BF16),
            pltpu.VMEM((layers, rows, cols), BF16),
            pltpu.VMEM((layers, groups, cap, cols), BF16),
            pltpu.VMEM((layers, rows, cols), BF16),
            pltpu.VMEM((layers, tok_rows, cols), BF16),
            pltpu.VMEM((layers, tok_rows, cols), BF16),
            DMA((layers,)), DMA((layers,)), DMA((layers,)),
            DMA((layers, groups)), DMA((layers, groups)),
            DMA((layers,)), DMA((layers,)),
        ],
        compiler_params=pltpu.CompilerParams(
            collective_id=2, has_side_effects=True, vmem_limit_bytes=56 * 2**20
        ),
        name="give_back",
    )(partials, mixing)


def on_device(
    tokens, pre_gain, route_ids, route_weights, gate_weight, up_weight, down_weight, post_gain
):
    tok_rows, cols = tokens.shape
    top_count = route_ids.shape[1]
    groups = lax.axis_size("ep")
    width = cols * lax.axis_size("tp")
    cap = 9 * tok_rows * top_count // (8 * groups)
    values = tokens.astype(jnp.float32)
    squares = sum_over_tp(jnp.sum(values * values, axis=1), 0)
    normed = (
        values * lax.rsqrt(squares / width + epsilon)[:, None] * pre_gain.astype(jnp.float32)[None, :]
    ).astype(BF16)

    experts = jnp.arange(groups, dtype=jnp.int32)
    named = route_ids[:, :, None] == experts[None, None, :]
    member = jnp.any(named, axis=1)
    weight = jnp.sum(jnp.where(named, route_weights[:, :, None], 0.0), axis=1)
    spot = jnp.arange(tok_rows, dtype=jnp.int32)
    before = (spot[:, None] > spot[None, :]).astype(BF16)
    rank = jnp.dot(before, member.astype(BF16), preferred_element_type=jnp.float32)
    key = jnp.where(member, rank.astype(jnp.int32), -1)
    slots = jnp.arange(cap, dtype=jnp.int32)
    table = (key.T[:, None, :] == slots[None, :, None]).astype(BF16)
    mixing = jnp.where(key[:, :, None] == slots[None, None, :], weight[:, :, None], 0.0)
    mixing = mixing.astype(BF16).reshape(tok_rows, groups * cap)

    piece = dispatch(normed, table)
    gate_act = jnp.dot(piece, gate_weight[0], preferred_element_type=jnp.float32)
    up_act = jnp.dot(piece, up_weight[0], preferred_element_type=jnp.float32)
    hidden = (jax.nn.silu(gate_act) * up_act).astype(BF16)
    partials = jnp.dot(hidden, down_weight[0], preferred_element_type=jnp.float32).astype(BF16)
    combined = give_back(partials, mixing, groups)
    totals = sum_over_tp(jnp.sum(combined * combined, axis=1), 3)
    scaled = combined * lax.rsqrt(totals / width + epsilon)[:, None]
    return (scaled * post_gain.astype(jnp.float32)[None, :]).astype(BF16)


def solution(mesh):
    placed = (
        P("ep", "tp"),
        P("tp"),
        P("ep", None),
        P("ep", None),
        P("ep", None, "tp"),
        P("ep", None, "tp"),
        P("ep", "tp", None),
        P("tp"),
    )
    return jax.shard_map(
        on_device, mesh=mesh, in_specs=placed, out_specs=P("ep", "tp"), check_vma=False
    )
```

```python
import functools

import jax
import jax.numpy as jnp
from jax import lax
from jax.experimental import pallas as pl
from jax.experimental.pallas import tpu as pltpu
from jax.sharding import PartitionSpec as P

epsilon = 1e-06
MESH = pl.DeviceIdType.MESH
DMA = pltpu.SemaphoreType.DMA
BF16 = jnp.bfloat16


def greet(targets):
    barrier = pltpu.get_barrier_semaphore()
    for target in targets:
        pl.semaphore_signal(barrier, inc=1, device_id=target, device_id_type=MESH)
    pl.semaphore_wait(barrier, len(targets))


def exchange_kernel(n, x_ref, out_ref, buf, send, recv):
    me = lax.axis_index("tp")
    peers = [{"tp": lax.rem(me + k, n)} for k in range(1, n)]
    greet(peers)
    copies = []
    for k in range(1, n):
        copy = pltpu.make_async_remote_copy(
            src_ref=x_ref, dst_ref=buf.at[k - 1], send_sem=send.at[k - 1],
            recv_sem=recv.at[k - 1], device_id=peers[k - 1], device_id_type=MESH,
        )
        copy.start()
        copies.append(copy)
    total = x_ref[...]
    for k in range(1, n):
        copies[k - 1].wait_recv()
        total = total + buf[k - 1]
    out_ref[...] = total
    for copy in copies:
        copy.wait_send()


def sum_over_tp(rows, number):
    n = lax.axis_size("tp")
    x = rows.reshape(-1, 128)
    total = pl.pallas_call(
        functools.partial(exchange_kernel, n),
        out_shape=jax.ShapeDtypeStruct(x.shape, jnp.float32),
        in_specs=[pl.BlockSpec(memory_space=pltpu.VMEM)],
        out_specs=pl.BlockSpec(memory_space=pltpu.VMEM),
        scratch_shapes=[pltpu.VMEM((n - 1,) + x.shape, jnp.float32), DMA((n - 1,)), DMA((n - 1,))],
        compiler_params=pltpu.CompilerParams(collective_id=number, has_side_effects=True),
        name="exchange%d" % number,
    )(x)
    return total.reshape(-1)


def places(groups, layers):
    me, g = lax.axis_index("tp"), lax.axis_index("ep")
    core, z = lax.rem(me, 2), me // 2
    return core, z, g, {"tp": me + 1 - 2 * core}


def greet_all(groups, layers, core, z, g, partner):
    targets = [partner]
    targets += [{"tp": lax.rem(z + k, layers) * 2 + core} for k in range(1, layers)]
    targets += [{"ep": lax.rem(g + m, groups)} for m in range(1, groups)]
    greet(targets)


def dispatch_kernel(
    groups, layers, cap, cols, tile, x_ref, key_ref, gate_ref, up_ref, out_ref,
    zbuf, obuf, sbuf, piece, wbuf, acc, zs, zr, es, er, ds, dr, ws,
):
    core, z, g, partner = places(groups, layers)
    loads = [
        pltpu.make_async_copy(ref, wbuf.at[i], ws.at[i]) for i, ref in enumerate((gate_ref, up_ref))
    ]
    for load in loads:
        load.start()
    greet_all(groups, layers, core, z, g, partner)

    def z_copy(k):
        return pltpu.make_async_remote_copy(
            src_ref=x_ref, dst_ref=zbuf.at[k], send_sem=zs.at[k], recv_sem=zr.at[k],
            device_id={"tp": lax.rem(z + k, layers) * 2 + core}, device_id_type=MESH,
        )

    def area(k, m):
        source = lax.rem(g + groups - m, groups)
        return piece.at[core, k, pl.ds(pl.multiple_of(source * cap, 16), cap)]

    def e_copy(k, m):
        return pltpu.make_async_remote_copy(
            src_ref=obuf.at[k, m], dst_ref=area(k, 0), send_sem=es.at[k, m],
            recv_sem=er.at[k, m], device_id={"ep": lax.rem(g + m, groups)}, device_id_type=MESH,
        )

    def d_copy(k, m):
        return pltpu.make_async_remote_copy(
            src_ref=area(k, m), dst_ref=area(k, m), send_sem=ds.at[k, m],
            recv_sem=dr.at[k, m], device_id=partner, device_id_type=MESH,
        )

    for k in range(1, layers):
        z_copy(k).start()
    zbuf[0] = x_ref[...]

    def build(e):
        wanted = lax.broadcasted_iota(jnp.int32, (cap, key_ref.shape[2]), 0)
        sbuf[e] = jnp.where(key_ref[e] == wanted, 1.0, 0.0).astype(BF16)

    def finish(k):
        @pl.loop(1, groups)
        def _(m):
            e_copy(k, m).wait_recv()
            d_copy(k, m).start()

        @pl.loop(0, groups)
        def _(m):
            d_copy(k, m).wait_recv()

        block = lax.rem(z + layers - k, layers)
        depth = pl.ds(pl.multiple_of(block * 2 * cols, 128), 2 * cols)

        @pl.loop(0, groups * cap // tile)
        def _(t):
            at = pl.ds(pl.multiple_of(t * tile, tile), tile)
            left = jnp.concatenate([piece[0, k, at], piece[1, k, at]], axis=1)
            gate = jnp.dot(left, wbuf[0, depth], preferred_element_type=jnp.float32)
            up = jnp.dot(left, wbuf[1, depth], preferred_element_type=jnp.float32)

            @pl.when(k == 0)
            def _():
                acc[0, at] = gate
                acc[1, at] = up

            @pl.when(jnp.logical_and(k > 0, k < layers - 1))
            def _():
                acc[0, at] += gate
                acc[1, at] += up

            @pl.when(k == layers - 1)
            def _():
                gates = acc[0, at] + gate
                out_ref[at] = (gates / (1.0 + jnp.exp(-gates)) * (acc[1, at] + up)).astype(BF16)

    @pl.loop(0, layers)
    def _(k):
        @pl.when(k > 0)
        def _():
            z_copy(k).wait_recv()

        @pl.loop(0, groups)
        def _(i):
            m = lax.rem(i + 1, groups)
            e = lax.rem(g + m, groups)

            @pl.when(k == 0)
            def _():
                build(e)

            tile_out = jnp.dot(sbuf[e], zbuf[k], preferred_element_type=jnp.float32).astype(BF16)

            @pl.when(m > 0)
            def _():
                obuf[k, m] = tile_out
                e_copy(k, m).start()

            @pl.when(m == 0)
            def _():
                piece[core, k, pl.ds(pl.multiple_of(g * cap, 16), cap)] = tile_out

        d_copy(k, 0).start()

        @pl.when(k == 1)
        def _():
            for load in loads:
                load.wait()

        @pl.when(k > 0)
        def _():
            finish(k - 1)

    finish(layers - 1)

    @pl.loop(0, layers)
    def _(k):
        @pl.when(k > 0)
        def _():
            z_copy(k).wait_send()

        @pl.loop(0, groups)
        def _(m):
            @pl.when(m > 0)
            def _():
                e_copy(k, m).wait_send()

            d_copy(k, m).wait_send()


def tile_of(rows, cap):
    return 384 if rows % 384 == 0 else cap


def dispatch(normed, key, cap, gate_weight, up_weight):
    tok_rows, groups = key.shape
    layers = lax.axis_size("tp") // 2
    cols = normed.shape[1]
    rows = groups * cap
    units = gate_weight.shape[1]
    vmem = pl.BlockSpec(memory_space=pltpu.VMEM)
    hbm = pl.BlockSpec(memory_space=pl.ANY)
    return pl.pallas_call(
        functools.partial(dispatch_kernel, groups, layers, cap, cols, tile_of(rows, cap)),
        out_shape=jax.ShapeDtypeStruct((rows, units), BF16),
        in_specs=[vmem, vmem, hbm, hbm],
        out_specs=vmem,
        scratch_shapes=[
            pltpu.VMEM((layers, tok_rows, cols), BF16),
            pltpu.VMEM((layers, groups, cap, cols), BF16),
            pltpu.VMEM((groups, cap, tok_rows), BF16),
            pltpu.VMEM((2, layers, rows, cols), BF16),
            pltpu.VMEM((2,) + gate_weight.shape, BF16),
            pltpu.VMEM((2, rows, units), jnp.float32),
            DMA((layers,)), DMA((layers,)),
            DMA((layers, groups)), DMA((layers, groups)),
            DMA((layers, groups)), DMA((layers, groups)),
            DMA((2,)),
        ],
        compiler_params=pltpu.CompilerParams(
            collective_id=1, has_side_effects=True, vmem_limit_bytes=60 * 2**20
        ),
        name="dispatch",
    )(normed, key.T.reshape(groups, 1, tok_rows), gate_weight, up_weight)


def return_kernel(
    groups, layers, cap, cols, tile, h_ref, down_ref, key_ref, weight_ref, out_ref,
    wbuf, mix, lbuf, sbuf, pbuf, qbuf, rbuf, obuf, fbuf, ws, ds, dr, es, er, zs, zr,
):
    core, z, g, partner = places(groups, layers)
    rows = groups * cap

    def w_copy(k, other):
        of = 1 - core if other else core
        column = (lax.rem(z + k, layers) * 2 + of) * cols
        return pltpu.make_async_copy(
            down_ref.at[:, pl.ds(pl.multiple_of(column, 128), cols)], wbuf.at[k, other], ws.at[k, other]
        )

    @pl.loop(0, layers)
    def _(i):
        k = lax.rem(i + 1, layers)
        w_copy(k, 1).start()
        w_copy(k, 0).start()

    greet_all(groups, layers, core, z, g, partner)

    def d_copy(k):
        return pltpu.make_async_remote_copy(
            src_ref=sbuf.at[k], dst_ref=pbuf.at[k], send_sem=ds.at[k],
            recv_sem=dr.at[k], device_id=partner, device_id_type=MESH,
        )

    def e_copy(k, m):
        return pltpu.make_async_remote_copy(
            src_ref=qbuf.at[k, m], dst_ref=rbuf.at[k, pl.ds(pl.multiple_of(g * cap, 16), cap)],
            send_sem=es.at[k, m], recv_sem=er.at[k, m],
            device_id={"ep": lax.rem(g + m, groups)}, device_id_type=MESH,
        )

    def z_copy(k):
        return pltpu.make_async_remote_copy(
            src_ref=obuf.at[k], dst_ref=fbuf.at[k], send_sem=zs.at[k], recv_sem=zr.at[k],
            device_id={"tp": lax.rem(z + k, layers) * 2 + core}, device_id_type=MESH,
        )

    def project(k, other, target):
        @pl.loop(0, rows // tile)
        def _(t):
            at = pl.ds(pl.multiple_of(t * tile, tile), tile)
            target[k, at] = jnp.dot(
                h_ref[at], wbuf[k, other], preferred_element_type=jnp.float32
            ).astype(BF16)

    @pl.loop(0, layers)
    def _(i):
        k = lax.rem(i + 1, layers)
        w_copy(k, 1).wait()
        project(k, 1, sbuf)
        d_copy(k).start()
        w_copy(k, 0).wait()
        project(k, 0, lbuf)
        d_copy(k).wait_recv()

        @pl.loop(0, groups)
        def _(j):
            m = lax.rem(j + 1, groups)
            at = pl.ds(pl.multiple_of(lax.rem(g + m, groups) * cap, 16), cap)
            both = lbuf[k, at].astype(jnp.float32) + pbuf[k, at].astype(jnp.float32)

            @pl.when(m > 0)
            def _():
                qbuf[k, m] = both.astype(BF16)
                e_copy(k, m).start()

            @pl.when(m == 0)
            def _():
                rbuf[k, pl.ds(pl.multiple_of(g * cap, 16), cap)] = both.astype(BF16)

        @pl.when(i == 0)
        def _():
            slots = lax.broadcasted_iota(jnp.int32, (mix.shape[1], cap), 1)
            for e in range(groups):
                mix[e] = jnp.where(
                    key_ref[:, e : e + 1] == slots, weight_ref[:, e : e + 1], 0.0
                ).astype(BF16)

    tok_rows = mix.shape[1]
    step = min(256, tok_rows)

    @pl.loop(0, layers)
    def _(i):
        k = lax.rem(i + 1, layers)

        @pl.loop(1, groups)
        def _(m):
            e_copy(k, m).wait_recv()

        @pl.loop(0, tok_rows // step)
        def _(t):
            at = pl.ds(pl.multiple_of(t * step, step), step)
            value = jnp.zeros((step, cols), jnp.float32)
            for e in range(groups):
                value += jnp.dot(
                    mix[e, at], rbuf[k, e * cap : (e + 1) * cap], preferred_element_type=jnp.float32
                )

            @pl.when(k > 0)
            def _():
                obuf[k, at] = value.astype(BF16)

            @pl.when(k == 0)
            def _():
                out_ref[at] = value

        @pl.when(k > 0)
        def _():
            z_copy(k).start()

    @pl.loop(1, layers)
    def _(k):
        z_copy(k).wait_recv()
        out_ref[...] += fbuf[k].astype(jnp.float32)

    @pl.loop(0, layers)
    def _(k):
        d_copy(k).wait_send()

        @pl.loop(1, groups)
        def _(m):
            e_copy(k, m).wait_send()

        @pl.when(k > 0)
        def _():
            z_copy(k).wait_send()


def give_back(hidden, down_weight, key, weight):
    rows, units = hidden.shape
    tok_rows, groups = key.shape
    layers = lax.axis_size("tp") // 2
    cols = down_weight.shape[1] // (2 * layers)
    cap = rows // groups
    vmem = pl.BlockSpec(memory_space=pltpu.VMEM)
    hbm = pl.BlockSpec(memory_space=pl.ANY)
    whole = pltpu.VMEM((layers, rows, cols), BF16)
    return pl.pallas_call(
        functools.partial(return_kernel, groups, layers, cap, cols, tile_of(rows, cap)),
        out_shape=jax.ShapeDtypeStruct((tok_rows, cols), jnp.float32),
        in_specs=[vmem, hbm, vmem, vmem],
        out_specs=vmem,
        scratch_shapes=[
            pltpu.VMEM((layers, 2, units, cols), BF16),
            pltpu.VMEM((groups, tok_rows, cap), BF16),
            whole, whole, whole,
            pltpu.VMEM((layers, groups, cap, cols), BF16),
            whole,
            pltpu.VMEM((layers, tok_rows, cols), BF16),
            pltpu.VMEM((layers, tok_rows, cols), BF16),
            DMA((layers, 2)), DMA((layers,)), DMA((layers,)),
            DMA((layers, groups)), DMA((layers, groups)),
            DMA((layers,)), DMA((layers,)),
        ],
        compiler_params=pltpu.CompilerParams(
            collective_id=2, has_side_effects=True, vmem_limit_bytes=60 * 2**20
        ),
        name="give_back",
    )(hidden, down_weight, key, weight)


def on_device(
    tokens, pre_gain, route_ids, route_weights, gate_weight, up_weight, down_weight, post_gain
):
    tok_rows, cols = tokens.shape
    top_count = route_ids.shape[1]
    groups = lax.axis_size("ep")
    width = cols * lax.axis_size("tp")
    cap = 9 * tok_rows * top_count // (8 * groups)
    values = tokens.astype(jnp.float32)
    squares = sum_over_tp(jnp.sum(values * values, axis=1), 0)
    normed = (
        values * lax.rsqrt(squares / width + epsilon)[:, None] * pre_gain.astype(jnp.float32)[None, :]
    ).astype(BF16)

    experts = jnp.arange(groups, dtype=jnp.int32)
    named = route_ids[:, :, None] == experts[None, None, :]
    member = jnp.any(named, axis=1)
    weight = jnp.sum(jnp.where(named, route_weights[:, :, None], 0.0), axis=1)
    spot = jnp.arange(tok_rows, dtype=jnp.int32)
    before = (spot[:, None] > spot[None, :]).astype(BF16)
    rank = jnp.dot(before, member.astype(BF16), preferred_element_type=jnp.float32)
    key = jnp.where(member, rank.astype(jnp.int32), -1)

    hidden = dispatch(normed, key, cap, gate_weight[0], up_weight[0])
    combined = give_back(hidden, down_weight[0], key, weight)
    totals = sum_over_tp(jnp.sum(combined * combined, axis=1), 3)
    scaled = combined * lax.rsqrt(totals / width + epsilon)[:, None]
    return (scaled * post_gain.astype(jnp.float32)[None, :]).astype(BF16)


def solution(mesh):
    placed = (
        P("ep", "tp"),
        P("tp"),
        P("ep", None),
        P("ep", None),
        P("ep", None, "tp"),
        P("ep", None, "tp"),
        P("ep", "tp", None),
        P("tp"),
    )
    return jax.shard_map(
        on_device, mesh=mesh, in_specs=placed, out_specs=P("ep", "tp"), check_vma=False
    )
```

```python
import functools

import jax
import jax.numpy as jnp
from jax import lax
from jax.experimental import pallas as pl
from jax.experimental.pallas import tpu as pltpu
from jax.sharding import PartitionSpec as P

epsilon = 1e-06
MESH = pl.DeviceIdType.MESH
DMA = pltpu.SemaphoreType.DMA
BF16 = jnp.bfloat16


def greet(targets):
    barrier = pltpu.get_barrier_semaphore()
    for target in targets:
        pl.semaphore_signal(barrier, inc=1, device_id=target, device_id_type=MESH)
    pl.semaphore_wait(barrier, len(targets))


def exchange_kernel(n, x_ref, out_ref, buf, send, recv):
    me = lax.axis_index("tp")
    peers = [{"tp": lax.rem(me + k, n)} for k in range(1, n)]
    greet(peers)
    copies = []
    for k in range(1, n):
        copy = pltpu.make_async_remote_copy(
            src_ref=x_ref, dst_ref=buf.at[k - 1], send_sem=send.at[k - 1],
            recv_sem=recv.at[k - 1], device_id=peers[k - 1], device_id_type=MESH,
        )
        copy.start()
        copies.append(copy)
    total = x_ref[...]
    for k in range(1, n):
        copies[k - 1].wait_recv()
        total = total + buf[k - 1]
    out_ref[...] = total
    for copy in copies:
        copy.wait_send()


def sum_over_tp(rows, number):
    n = lax.axis_size("tp")
    x = rows.reshape(-1, 128)
    total = pl.pallas_call(
        functools.partial(exchange_kernel, n),
        out_shape=jax.ShapeDtypeStruct(x.shape, jnp.float32),
        in_specs=[pl.BlockSpec(memory_space=pltpu.VMEM)],
        out_specs=pl.BlockSpec(memory_space=pltpu.VMEM),
        scratch_shapes=[pltpu.VMEM((n - 1,) + x.shape, jnp.float32), DMA((n - 1,)), DMA((n - 1,))],
        compiler_params=pltpu.CompilerParams(collective_id=number, has_side_effects=True),
        name="exchange%d" % number,
    )(x)
    return total.reshape(-1)


def places(groups, layers):
    me, g = lax.axis_index("tp"), lax.axis_index("ep")
    core, z = lax.rem(me, 2), me // 2
    return core, z, g, {"tp": me + 1 - 2 * core}


def greet_all(groups, layers, core, z, g, partner):
    targets = [partner]
    targets += [{"tp": lax.rem(z + k, layers) * 2 + core} for k in range(1, layers)]
    targets += [{"ep": lax.rem(g + m, groups)} for m in range(1, groups)]
    greet(targets)


def dispatch_kernel(
    groups, layers, cap, cols, tile, x_ref, key_ref, gate_ref, up_ref, out_ref,
    zbuf, obuf, sbuf, piece, wbuf, acc, zs, zr, es, er, ds, dr, ws,
):
    core, z, g, partner = places(groups, layers)
    loads = [
        pltpu.make_async_copy(ref, wbuf.at[i], ws.at[i]) for i, ref in enumerate((gate_ref, up_ref))
    ]
    for load in loads:
        load.start()
    greet_all(groups, layers, core, z, g, partner)

    def z_copy(source, to, at, sem):
        return pltpu.make_async_remote_copy(
            src_ref=source, dst_ref=zbuf.at[at], send_sem=zs.at[sem], recv_sem=zr.at[at],
            device_id={"tp": to * 2 + core}, device_id_type=MESH,
        )

    def slot(s):
        inner = jnp.minimum(z, layers - 1 - z)
        near = jnp.where(s % 2 == 1, (s + 1) // 2, layers - (s + 1) // 2)
        far = jnp.where(2 * z > layers - 1, s - inner, layers - s + inner)
        return jnp.where(s == 0, 0, jnp.where(s <= 2 * inner, near, far))

    to_right = z_copy(x_ref, z + 1, 1, 0)
    to_left = z_copy(x_ref, z - 1, layers - 1, layers)

    def relays(k):
        right = jnp.logical_and(jnp.logical_and(k > 0, z >= k), z < layers - 1)
        left = jnp.logical_and(z < k, z > 0)
        return (
            (right, z_copy(zbuf.at[k], z + 1, k + 1, k)),
            (left, z_copy(zbuf.at[k], z - 1, k - 1, k)),
        )

    def area(k, m):
        source = lax.rem(g + groups - m, groups)
        return piece.at[core, k, pl.ds(pl.multiple_of(source * cap, 16), cap)]

    def e_copy(k, m):
        return pltpu.make_async_remote_copy(
            src_ref=obuf.at[k, m], dst_ref=area(k, 0), send_sem=es.at[k, m],
            recv_sem=er.at[k, m], device_id={"ep": lax.rem(g + m, groups)}, device_id_type=MESH,
        )

    def d_copy(k, m):
        return pltpu.make_async_remote_copy(
            src_ref=area(k, m), dst_ref=area(k, m), send_sem=ds.at[k, m],
            recv_sem=dr.at[k, m], device_id=partner, device_id_type=MESH,
        )

    pl.when(z < layers - 1)(to_right.start)
    pl.when(z > 0)(to_left.start)
    zbuf[0] = x_ref[...]

    def build(e):
        wanted = lax.broadcasted_iota(jnp.int32, (cap, key_ref.shape[2]), 0)
        sbuf[e] = jnp.where(key_ref[e] == wanted, 1.0, 0.0).astype(BF16)

    def finish(s):
        k = slot(s)

        @pl.loop(1, groups)
        def _(m):
            e_copy(k, m).wait_recv()
            d_copy(k, m).start()

        @pl.loop(0, groups)
        def _(m):
            d_copy(k, m).wait_recv()

        block = lax.rem(z + layers - k, layers)
        depth = pl.ds(pl.multiple_of(block * 2 * cols, 128), 2 * cols)

        @pl.loop(0, groups * cap // tile)
        def _(t):
            at = pl.ds(pl.multiple_of(t * tile, tile), tile)
            left = jnp.concatenate([piece[0, k, at], piece[1, k, at]], axis=1)
            gate = jnp.dot(left, wbuf[0, depth], preferred_element_type=jnp.float32)
            up = jnp.dot(left, wbuf[1, depth], preferred_element_type=jnp.float32)

            @pl.when(s == 0)
            def _():
                acc[0, at] = gate
                acc[1, at] = up

            @pl.when(jnp.logical_and(s > 0, s < layers - 1))
            def _():
                acc[0, at] += gate
                acc[1, at] += up

            @pl.when(s == layers - 1)
            def _():
                gates = acc[0, at] + gate
                out_ref[at] = (gates / (1.0 + jnp.exp(-gates)) * (acc[1, at] + up)).astype(BF16)

    @pl.loop(0, layers)
    def _(s):
        k = slot(s)

        @pl.when(s > 0)
        def _():
            z_copy(x_ref, lax.rem(z + 1, layers), k, k).wait_recv()
            for wanted, copy in relays(k):
                pl.when(wanted)(copy.start)

        @pl.loop(0, groups)
        def _(i):
            m = lax.rem(i + 1, groups)
            e = lax.rem(g + m, groups)

            @pl.when(s == 0)
            def _():
                build(e)

            tile_out = jnp.dot(sbuf[e], zbuf[k], preferred_element_type=jnp.float32).astype(BF16)

            @pl.when(m > 0)
            def _():
                obuf[k, m] = tile_out
                e_copy(k, m).start()

            @pl.when(m == 0)
            def _():
                piece[core, k, pl.ds(pl.multiple_of(g * cap, 16), cap)] = tile_out

        d_copy(k, 0).start()

        @pl.when(s == 1)
        def _():
            for load in loads:
                load.wait()

        @pl.when(s > 0)
        def _():
            finish(s - 1)

    finish(layers - 1)
    pl.when(z < layers - 1)(to_right.wait_send)
    pl.when(z > 0)(to_left.wait_send)

    @pl.loop(0, layers)
    def _(k):
        for wanted, copy in relays(k):
            pl.when(wanted)(copy.wait_send)

        @pl.loop(0, groups)
        def _(m):
            @pl.when(m > 0)
            def _():
                e_copy(k, m).wait_send()

            d_copy(k, m).wait_send()


def tile_of(rows, cap):
    return 384 if rows % 384 == 0 else cap


def dispatch(normed, key, cap, gate_weight, up_weight):
    tok_rows, groups = key.shape
    layers = lax.axis_size("tp") // 2
    cols = normed.shape[1]
    rows = groups * cap
    units = gate_weight.shape[1]
    vmem = pl.BlockSpec(memory_space=pltpu.VMEM)
    hbm = pl.BlockSpec(memory_space=pl.ANY)
    return pl.pallas_call(
        functools.partial(dispatch_kernel, groups, layers, cap, cols, tile_of(rows, cap)),
        out_shape=jax.ShapeDtypeStruct((rows, units), BF16),
        in_specs=[vmem, vmem, hbm, hbm],
        out_specs=vmem,
        scratch_shapes=[
            pltpu.VMEM((layers, tok_rows, cols), BF16),
            pltpu.VMEM((layers, groups, cap, cols), BF16),
            pltpu.VMEM((groups, cap, tok_rows), BF16),
            pltpu.VMEM((2, layers, rows, cols), BF16),
            pltpu.VMEM((2,) + gate_weight.shape, BF16),
            pltpu.VMEM((2, rows, units), jnp.float32),
            DMA((layers + 1,)), DMA((layers,)),
            DMA((layers, groups)), DMA((layers, groups)),
            DMA((layers, groups)), DMA((layers, groups)),
            DMA((2,)),
        ],
        compiler_params=pltpu.CompilerParams(
            collective_id=1, has_side_effects=True, vmem_limit_bytes=60 * 2**20
        ),
        name="dispatch",
    )(normed, key.T.reshape(groups, 1, tok_rows), gate_weight, up_weight)


def return_kernel(
    groups, layers, cap, cols, tile, h_ref, down_ref, key_ref, weight_ref, out_ref,
    wbuf, mix, lbuf, sbuf, pbuf, qbuf, rbuf, obuf, fbuf, ws, ds, dr, es, er, zs, zr,
):
    core, z, g, partner = places(groups, layers)
    rows = groups * cap

    def w_copy(k, other):
        of = 1 - core if other else core
        column = (lax.rem(z + k, layers) * 2 + of) * cols
        return pltpu.make_async_copy(
            down_ref.at[:, pl.ds(pl.multiple_of(column, 128), cols)], wbuf.at[k, other], ws.at[k, other]
        )

    @pl.loop(0, layers)
    def _(i):
        k = lax.rem(i + 1, layers)
        w_copy(k, 1).start()
        w_copy(k, 0).start()

    greet_all(groups, layers, core, z, g, partner)

    def d_copy(k):
        return pltpu.make_async_remote_copy(
            src_ref=sbuf.at[k], dst_ref=pbuf.at[k], send_sem=ds.at[k],
            recv_sem=dr.at[k], device_id=partner, device_id_type=MESH,
        )

    def e_copy(k, m):
        return pltpu.make_async_remote_copy(
            src_ref=qbuf.at[k, m], dst_ref=rbuf.at[k, pl.ds(pl.multiple_of(g * cap, 16), cap)],
            send_sem=es.at[k, m], recv_sem=er.at[k, m],
            device_id={"ep": lax.rem(g + m, groups)}, device_id_type=MESH,
        )

    def z_copy(k):
        return pltpu.make_async_remote_copy(
            src_ref=obuf.at[k], dst_ref=fbuf.at[k], send_sem=zs.at[k], recv_sem=zr.at[k],
            device_id={"tp": lax.rem(z + k, layers) * 2 + core}, device_id_type=MESH,
        )

    def project(k, other, target):
        @pl.loop(0, rows // tile)
        def _(t):
            at = pl.ds(pl.multiple_of(t * tile, tile), tile)
            target[k, at] = jnp.dot(
                h_ref[at], wbuf[k, other], preferred_element_type=jnp.float32
            ).astype(BF16)

    @pl.loop(0, layers)
    def _(i):
        k = lax.rem(i + 1, layers)
        w_copy(k, 1).wait()
        project(k, 1, sbuf)
        d_copy(k).start()
        w_copy(k, 0).wait()
        project(k, 0, lbuf)
        d_copy(k).wait_recv()

        @pl.loop(0, groups)
        def _(j):
            m = lax.rem(j + 1, groups)
            at = pl.ds(pl.multiple_of(lax.rem(g + m, groups) * cap, 16), cap)
            both = lbuf[k, at].astype(jnp.float32) + pbuf[k, at].astype(jnp.float32)

            @pl.when(m > 0)
            def _():
                qbuf[k, m] = both.astype(BF16)
                e_copy(k, m).start()

            @pl.when(m == 0)
            def _():
                rbuf[k, pl.ds(pl.multiple_of(g * cap, 16), cap)] = both.astype(BF16)

        @pl.when(i == 0)
        def _():
            slots = lax.broadcasted_iota(jnp.int32, (mix.shape[1], cap), 1)
            for e in range(groups):
                mix[e] = jnp.where(
                    key_ref[:, e : e + 1] == slots, weight_ref[:, e : e + 1], 0.0
                ).astype(BF16)

    tok_rows = mix.shape[1]
    step = min(256, tok_rows)

    @pl.loop(0, layers)
    def _(i):
        k = lax.rem(i + 1, layers)

        @pl.loop(1, groups)
        def _(m):
            e_copy(k, m).wait_recv()

        @pl.loop(0, tok_rows // step)
        def _(t):
            at = pl.ds(pl.multiple_of(t * step, step), step)
            value = jnp.zeros((step, cols), jnp.float32)
            for e in range(groups):
                value += jnp.dot(
                    mix[e, at], rbuf[k, e * cap : (e + 1) * cap], preferred_element_type=jnp.float32
                )

            @pl.when(k > 0)
            def _():
                obuf[k, at] = value.astype(BF16)

            @pl.when(k == 0)
            def _():
                out_ref[at] = value

        @pl.when(k > 0)
        def _():
            z_copy(k).start()

    @pl.loop(1, layers)
    def _(k):
        z_copy(k).wait_recv()
        out_ref[...] += fbuf[k].astype(jnp.float32)

    @pl.loop(0, layers)
    def _(k):
        d_copy(k).wait_send()

        @pl.loop(1, groups)
        def _(m):
            e_copy(k, m).wait_send()

        @pl.when(k > 0)
        def _():
            z_copy(k).wait_send()


def give_back(hidden, down_weight, key, weight):
    rows, units = hidden.shape
    tok_rows, groups = key.shape
    layers = lax.axis_size("tp") // 2
    cols = down_weight.shape[1] // (2 * layers)
    cap = rows // groups
    vmem = pl.BlockSpec(memory_space=pltpu.VMEM)
    hbm = pl.BlockSpec(memory_space=pl.ANY)
    whole = pltpu.VMEM((layers, rows, cols), BF16)
    return pl.pallas_call(
        functools.partial(return_kernel, groups, layers, cap, cols, tile_of(rows, cap)),
        out_shape=jax.ShapeDtypeStruct((tok_rows, cols), jnp.float32),
        in_specs=[vmem, hbm, vmem, vmem],
        out_specs=vmem,
        scratch_shapes=[
            pltpu.VMEM((layers, 2, units, cols), BF16),
            pltpu.VMEM((groups, tok_rows, cap), BF16),
            whole, whole, whole,
            pltpu.VMEM((layers, groups, cap, cols), BF16),
            whole,
            pltpu.VMEM((layers, tok_rows, cols), BF16),
            pltpu.VMEM((layers, tok_rows, cols), BF16),
            DMA((layers, 2)), DMA((layers,)), DMA((layers,)),
            DMA((layers, groups)), DMA((layers, groups)),
            DMA((layers,)), DMA((layers,)),
        ],
        compiler_params=pltpu.CompilerParams(
            collective_id=2, has_side_effects=True, vmem_limit_bytes=60 * 2**20
        ),
        name="give_back",
    )(hidden, down_weight, key, weight)


def on_device(
    tokens, pre_gain, route_ids, route_weights, gate_weight, up_weight, down_weight, post_gain
):
    tok_rows, cols = tokens.shape
    top_count = route_ids.shape[1]
    groups = lax.axis_size("ep")
    width = cols * lax.axis_size("tp")
    cap = 9 * tok_rows * top_count // (8 * groups)
    values = tokens.astype(jnp.float32)
    squares = sum_over_tp(jnp.sum(values * values, axis=1), 0)
    normed = (
        values * lax.rsqrt(squares / width + epsilon)[:, None] * pre_gain.astype(jnp.float32)[None, :]
    ).astype(BF16)

    experts = jnp.arange(groups, dtype=jnp.int32)
    named = route_ids[:, :, None] == experts[None, None, :]
    member = jnp.any(named, axis=1)
    weight = jnp.sum(jnp.where(named, route_weights[:, :, None], 0.0), axis=1)
    spot = jnp.arange(tok_rows, dtype=jnp.int32)
    before = (spot[:, None] > spot[None, :]).astype(BF16)
    rank = jnp.dot(before, member.astype(BF16), preferred_element_type=jnp.float32)
    key = jnp.where(member, rank.astype(jnp.int32), -1)

    hidden = dispatch(normed, key, cap, gate_weight[0], up_weight[0])
    combined = give_back(hidden, down_weight[0], key, weight)
    totals = sum_over_tp(jnp.sum(combined * combined, axis=1), 3)
    scaled = combined * lax.rsqrt(totals / width + epsilon)[:, None]
    return (scaled * post_gain.astype(jnp.float32)[None, :]).astype(BF16)


def solution(mesh):
    placed = (
        P("ep", "tp"),
        P("tp"),
        P("ep", None),
        P("ep", None),
        P("ep", None, "tp"),
        P("ep", None, "tp"),
        P("ep", "tp", None),
        P("tp"),
    )
    return jax.shard_map(
        on_device, mesh=mesh, in_specs=placed, out_specs=P("ep", "tp"), check_vma=False
    )
```
